32 devices in a mesh: ep: 8 (over z, x), tp: 4 (over y, core).
Axes of the slice: x: 2, y: 2, z: 4, core: 2. Of those that a mesh axis runs over, the one named last changes fastest.
Arguments:
- tokens: bfloat16 [64, 2048], P('ep'), may hold values from -6 to 6
- mix_gain: bfloat16 [2048], replicated, may hold values from 0.099609375 to 1.8984375
- w_query: bfloat16 [2048, 512], P(None, 'tp'), may hold values from -0.125 to 0.125
- w_key: bfloat16 [2048, 512], P(None, 'tp'), may hold values from -0.125 to 0.125
- w_value: bfloat16 [2048, 512], P(None, 'tp'), may hold values from -0.125 to 0.125
- w_igate: bfloat16 [2048, 4], replicated, may hold values from -0.125 to 0.125
- w_fgate: bfloat16 [2048, 4], replicated, may hold values from -0.125 to 0.125
- forget_bias: float32 [4], replicated, may hold values from 0.5 to 4.5
- w_out: bfloat16 [512, 2048], P('tp'), may hold values from -0.25 to 0.25
- mem_state: float32 [64, 4, 16384], P('ep', 'tp'), may hold values from -0.75 to 0.75
- norm_state: float32 [64, 512], P('ep', 'tp'), may hold values from -0.75 to 0.75
- max_state: float32 [64, 4], P('ep', 'tp'), may hold values from -3 to 3
- ffn_gain: bfloat16 [2048], replicated, may hold values from 0.099609375 to 1.8984375
- route_ids: int32 [64, 2], P('ep'), may hold values from 0 to 7, all different within a row; in each aligned block of 8 rows (0 to 7, 8 to 15, ...) at most 3 rows name the same one
- route_weights: float32 [64, 2], P('ep'), may hold values from 0.1 to 1
- w_gate: bfloat16 [2048, 32768], P(None, ('ep', 'tp')), may hold values from -0.125 to 0.125
- w_up: bfloat16 [2048, 32768], P(None, ('ep', 'tp')), may hold values from -0.125 to 0.125
- w_down: bfloat16 [32768, 2048], P('ep', 'tp'), may hold values from -0.09375 to 0.09375
Outputs:
- out_tokens: bfloat16 [64, 2048], P('ep', 'tp')
- new_memory: float32 [64, 4, 16384], P('ep', 'tp')
- new_norm: float32 [64, 512], P('ep', 'tp')
- new_max: float32 [64, 4], P('ep', 'tp')
The draws below stay inside these ranges and needn't reach their ends.
Inputs may be any that keep to these rules, and one draw needn't show every extreme that they name: `route_ids`: each row names 2 different experts; among the rows of one index of ep no expert is named more than 3 times, a bound that some block reaches.
All inputs are finite; a program needn't handle non-finite values.
Results may differ from the reference program's by a relative error of at most 0.013.
The reference program's roundings to bfloat16 on the way (of `normed`, `query_rows`, `readout`, `residual`, `normed_ffn` and `hidden`) count: a program that leaves them out, or rounds other values in their place, can miss the bound.
Values may be sent and summed in bfloat16 or wider, within the bound.
A program may use at most 64 MiB of HBM per device.

```python
import math
import jax
import jax.numpy as jnp
import numpy as np
from jax import lax

D = 2048
HEADS = 4
HEAD_DIM = 128
FF = 4096
TOPK = 2
SEQ_DEV = 8
EXPERTS = 8
CAP = 3
BATCH = 64
N_EP = 8
N_TP = 4


def steps_of(stream_key, shape, pieces, low, top_value):
    factor_of, own = 1.0, jax.random.fold_in(stream_key, 6)
    for dim, parts in pieces:
        heights = jnp.exp(jax.random.uniform(jax.random.fold_in(own, dim), (parts,), jnp.float32, low / len(pieces), top_value / len(pieces)))
        factor_of = factor_of * jnp.repeat(heights, shape[dim] // parts).reshape([-1 if axis == dim else 1 for axis in range(len(shape))])
    return factor_of


def assign_block(own_key, own, number, rows, number_of, top, limit, slope):
    ranking = jax.random.permutation(own_key, number_of)
    packed, ordinary = portions_of(number_of, rows * top, limit, slope, True), portions_of(number_of, rows * top, limit, slope, False)
    places = jnp.arange(number_of)

    def named(lengths, offset_by):
        used = int((lengths > 0).sum())
        fixed = max(1, used // 4)
        shifted = fixed + (places - fixed + offset_by * (used - fixed)) % max(1, number_of - fixed)
        return jnp.zeros((number_of,), jnp.int32).at[ranking[jnp.where(places < fixed, places, shifted)]].set(jnp.asarray(lengths, jnp.int32))

    lengths = jnp.where(number % 4 == 0, named(packed, number // 4), named(ordinary, number - number // 4 - 1))
    mixed = jax.random.permutation(jax.random.fold_in(own, 3), number_of)
    donor, sink = mixed[0:number_of // 2 * 2:2], mixed[1:number_of // 2 * 2:2]
    slack = jnp.minimum(lengths[donor] - 1, limit - lengths[sink]) // 2
    slack = jnp.where((donor == ranking[0]) | (sink == ranking[0]) | (lengths[sink] == 0), 0, jnp.maximum(slack, 0))
    shifted = jax.random.randint(jax.random.fold_in(own, 4), (number_of // 2,), 0, 1 << 20) % (slack + 1)
    lengths = lengths.at[donor].add(-shifted).at[sink].add(shifted)
    items = jnp.searchsorted(jnp.cumsum(lengths), jnp.arange(rows * top), side="right").astype(jnp.int32)
    grid = items.reshape(top, rows).T
    grid = grid[jax.random.permutation(jax.random.fold_in(own, 1), rows)]
    offset_by = jax.random.randint(jax.random.fold_in(own, 2), (rows, 1), 0, top)
    return jnp.take_along_axis(grid, (jnp.arange(top)[None, :] + offset_by) % top, axis=1)


def portions_of(number_of, total, most, lean, full):
    weights = [(1 << 20) // math.isqrt(rank ** lean) + 1 for rank in range(1, number_of + 1)]
    largest = most if full else min(most, max(-(-total // number_of), total * weights[0] // sum(weights)))
    least = 1 if total - largest >= number_of - 1 else 0
    given, surplus = [largest] + [least] * (number_of - 1), total - largest - least * (number_of - 1)
    while surplus > 0:
        free = [i for i in range(1, number_of) if given[i] < largest] or [i for i in range(1, number_of) if given[i] < most]
        whole, budget = sum([weights[i] for i in free]), surplus
        for i in free:
            more = min(most - given[i], max(1, budget * weights[i] // whole), surplus)
            given[i] = given[i] + more
            surplus = surplus - more
    return np.array(given)


def gaussian(stream_key, shape, scale, most, pieces=(), held_as=jnp.bfloat16):
    factor_of = steps_of(stream_key, shape, pieces, -0.22, 0.18) if pieces else 1.0
    result = jax.random.normal(stream_key, shape, jnp.float32) * scale * factor_of
    return jnp.minimum(jnp.maximum(result, -most), most).astype(held_as)


def setup_inputs(seed: int = 0) -> dict:
    keys = jax.random.split(jax.random.key(seed), 19)
    tokens = gaussian(keys[0], (BATCH, D), 1.0, 6.0, ((0, 8),))
    mix_gain = jnp.clip(1.0 + 0.18 * jax.random.normal(keys[1], (D,), jnp.float32), 0.099609375, 1.8984375).astype(jnp.bfloat16)
    w_query = gaussian(keys[2], (D, HEADS * HEAD_DIM), D ** -0.5, 0.125, ((1, 4),))
    w_key = gaussian(keys[3], (D, HEADS * HEAD_DIM), D ** -0.5, 0.125, ((1, 4),))
    w_value = gaussian(keys[4], (D, HEADS * HEAD_DIM), D ** -0.5, 0.125, ((1, 4),))
    w_igate = gaussian(keys[5], (D, HEADS), D ** -0.5, 0.125)
    w_fgate = gaussian(keys[6], (D, HEADS), D ** -0.5, 0.125)
    forget_bias = jnp.clip(jax.random.uniform(keys[7], (HEADS,), jnp.float32, 0.5, 4.5), 0.5, 4.5)
    w_out = gaussian(keys[8], (HEADS * HEAD_DIM, D), (HEADS * HEAD_DIM) ** -0.5, 0.25, ((0, 4),))
    mem_state = gaussian(keys[9], (BATCH, HEADS, HEAD_DIM * HEAD_DIM), 0.125, 0.75, ((0, 8), (1, 4)), jnp.float32)
    norm_state = gaussian(keys[10], (BATCH, HEADS * HEAD_DIM), 0.125, 0.75, ((0, 8), (1, 4)), jnp.float32)
    max_state = jnp.clip(jax.random.uniform(keys[11], (BATCH, HEADS), jnp.float32, -3.0, 3.0) * steps_of(keys[11], (BATCH, HEADS), ((0, 8), (1, 4)), -0.4, 0.0), -3.0, 3.0)
    ffn_gain = jnp.clip(1.0 + 0.18 * jax.random.normal(keys[12], (D,), jnp.float32), 0.099609375, 1.8984375).astype(jnp.bfloat16)
    route_ids_keys = jax.random.split(jax.random.fold_in(keys[13], 1), BATCH // SEQ_DEV)
    route_ids_turns = jax.random.permutation(jax.random.fold_in(keys[13], 3), BATCH // SEQ_DEV)
    route_ids = jax.vmap(lambda own, number: assign_block(jax.random.fold_in(keys[13], 2), own, number, SEQ_DEV, EXPERTS, TOPK, CAP, 2))(route_ids_keys, route_ids_turns).reshape((BATCH, TOPK))
    route_weights = jnp.clip(jnp.exp(math.log(1.0) - 2.3025851 * jax.random.uniform(keys[14], (BATCH, TOPK), jnp.float32) ** steps_of(keys[14], (BATCH, TOPK), ((0, 8),), -0.2, 0.2)), 0.1, 1.0)
    w_gate = gaussian(keys[15], (D, EXPERTS * FF), D ** -0.5, 0.125, ((1, 32),))
    w_up = gaussian(keys[16], (D, EXPERTS * FF), D ** -0.5, 0.125, ((1, 32),))
    w_down = gaussian(keys[17], (EXPERTS * FF, D), FF ** -0.5, 0.09375, ((0, 8), (1, 4)))
    return dict(tokens=tokens, mix_gain=mix_gain, w_query=w_query, w_key=w_key, w_value=w_value, w_igate=w_igate, w_fgate=w_fgate, forget_bias=forget_bias, w_out=w_out, mem_state=mem_state, norm_state=norm_state, max_state=max_state, ffn_gain=ffn_gain, route_ids=route_ids, route_weights=route_weights, w_gate=w_gate, w_up=w_up, w_down=w_down)


epsilon = 1e-06

def scaled_rows(row_data, gain_values):
    squares = lax.optimization_barrier(jnp.mean(row_data * row_data, axis=1, keepdims=True))
    return (row_data * lax.rsqrt(squares + epsilon) * gain_values.astype(jnp.float32)).astype(jnp.bfloat16)

def rounded_wide(matrix):
    return lax.optimization_barrier(matrix.astype(jnp.bfloat16)).astype(jnp.float32)

def reference(tokens, mix_gain, w_query, w_key, w_value, w_igate, w_fgate, forget_bias, w_out, mem_state, norm_state, max_state, ffn_gain, route_ids, route_weights, w_gate, w_up, w_down):
    residual_in = tokens.astype(jnp.float32)
    normed = scaled_rows(residual_in, mix_gain)
    query_rows = rounded_wide(jnp.dot(normed, w_query, preferred_element_type=jnp.float32)).reshape(BATCH, HEADS, HEAD_DIM)
    key_rows = rounded_wide(jnp.dot(normed, w_key, preferred_element_type=jnp.float32)).reshape(BATCH, HEADS, HEAD_DIM)
    key_rows = key_rows * HEAD_DIM ** (-0.5)
    value_rows = rounded_wide(jnp.dot(normed, w_value, preferred_element_type=jnp.float32)).reshape(BATCH, HEADS, HEAD_DIM)
    input_gate = jnp.dot(normed, w_igate, preferred_element_type=jnp.float32)
    forget_log = jax.nn.log_sigmoid(jnp.dot(normed, w_fgate, preferred_element_type=jnp.float32) + forget_bias[None, :])
    new_max = jnp.maximum(forget_log + max_state, input_gate)
    keep_weight = jnp.exp(forget_log + max_state - new_max)
    new_weight = jnp.exp(input_gate - new_max)
    memory = mem_state.reshape(BATCH, HEADS, HEAD_DIM, HEAD_DIM)
    new_memory = keep_weight[:, :, None, None] * memory + new_weight[:, :, None, None] * key_rows[:, :, :, None] * value_rows[:, :, None, :]
    new_norm = keep_weight[:, :, None] * norm_state.reshape(BATCH, HEADS, HEAD_DIM) + new_weight[:, :, None] * key_rows
    numerator = jnp.einsum('bhd,bhde->bhe', query_rows, new_memory, precision=lax.Precision.HIGHEST)
    denominator = lax.optimization_barrier(jnp.sum(query_rows * new_norm, axis=2))
    readout = (numerator / jnp.maximum(jnp.abs(denominator), jnp.exp(-new_max))[:, :, None]).astype(jnp.bfloat16)
    readout = readout.reshape(BATCH, HEADS * HEAD_DIM)
    group_width = HEADS * HEAD_DIM // N_TP
    head_total = jnp.zeros((BATCH, D), jnp.float32)
    for group_at in range(N_TP):
        group_start = group_at * group_width
        product = jnp.dot(readout[:, group_start:group_start + group_width], w_out[group_start:group_start + group_width], preferred_element_type=jnp.float32)
        head_total = head_total + rounded_wide(product)
    residual = (residual_in + head_total).astype(jnp.bfloat16)
    residual_wide = lax.optimization_barrier(residual).astype(jnp.float32)
    normed_ffn = scaled_rows(residual_wide, ffn_gain)
    route_bound = N_EP * CAP
    flat_ids = route_ids.reshape(-1)
    flat_weights = route_weights.reshape(-1)

    def one_expert(running, expert_at):
        matches = flat_ids == expert_at
        places = jnp.nonzero(matches, size=route_bound, fill_value=0)[0].astype(jnp.int32)
        live = (jnp.arange(route_bound, dtype=jnp.int32) < jnp.sum(matches.astype(jnp.int32))).astype(jnp.float32)
        token_at = places // TOPK
        picked = jnp.take(normed_ffn, token_at, axis=0)
        start = (expert_at * FF).astype(jnp.int32)
        gate_sum = jnp.dot(picked, lax.dynamic_slice_in_dim(w_gate, start, FF, 1), preferred_element_type=jnp.float32)
        up_sum = jnp.dot(picked, lax.dynamic_slice_in_dim(w_up, start, FF, 1), preferred_element_type=jnp.float32)
        hidden = (jax.nn.silu(gate_sum) * up_sum).astype(jnp.bfloat16)
        expert_out = jnp.dot(hidden, lax.dynamic_slice_in_dim(w_down, start, FF, 0), preferred_element_type=jnp.float32)
        scale = jnp.take(flat_weights, places) * live
        return (running.at[token_at].add(expert_out * scale[:, None]), None)
    routed, unused = lax.scan(one_expert, jnp.zeros((BATCH, D), jnp.float32), jnp.arange(EXPERTS, dtype=jnp.int32))
    out_tokens = (residual_wide + routed).astype(jnp.bfloat16)
    return (out_tokens, new_memory.reshape(BATCH, HEADS, HEAD_DIM * HEAD_DIM), new_norm.reshape(BATCH, HEADS * HEAD_DIM), new_max)
```

```python
import functools

import jax
import jax.numpy as jnp
from jax import lax
from jax.experimental import pallas as pl
from jax.experimental.pallas import tpu as pltpu
from jax.sharding import PartitionSpec as P

FF = 4096
epsilon = 1e-06
MESH = pl.DeviceIdType.MESH
F32 = jnp.float32
BF16 = jnp.bfloat16


def normalized(rows, gain):
    squares = jnp.sum(rows * rows, axis=1, keepdims=True) / rows.shape[1]
    return (rows * lax.rsqrt(squares + epsilon) * gain).astype(BF16)


def merged(ref, count):
    return jnp.concatenate([ref[i].astype(F32) for i in range(count)], axis=0)


def kernel(
    sizes,
    tokens,
    mix_gain,
    igate_rows,
    fgate_rows,
    forget_bias,
    norm_state,
    max_row,
    ffn_gain,
    ids,
    route_w,
    w_query,
    w_key,
    w_value,
    w_out,
    mem_state,
    w_gate,
    w_up,
    w_down,
    out_tokens,
    new_memory,
    new_norm,
    new_max_row,
    qkv_buf,
    out_buf,
    mem_buf,
    gate_buf,
    up_buf,
    down_buf,
    parts,
    residual_buf,
    packed,
    arrived,
    hidden_all,
    back,
    returned,
    load_sem,
    mem_sem,
    part_send,
    part_recv,
    row_send,
    row_recv,
    hid_send,
    hid_recv,
    back_send,
    back_recv,
):
    tp_count, ep_count, span, experts, slots, heads = sizes
    tp_at = lax.axis_index("tp")
    ep_at = lax.axis_index("ep")
    seqs, width = tokens.shape
    head_dim = mem_buf.shape[-1]
    own_width = out_tokens.shape[1]

    def load(src, dst, at):
        copy = pltpu.make_async_copy(src, dst, load_sem.at[at])
        copy.start()
        return copy

    loads = [load(w, qkv_buf.at[i], i) for i, w in enumerate((w_query, w_key, w_value))]
    load_mem = load(mem_state, mem_buf, 3)
    load_out = load(w_out, out_buf, 4)
    load_gate = load(w_gate, gate_buf, 5)
    load_up = load(w_up, up_buf, 6)
    load_down = load(w_down, down_buf, 7)

    barrier = pltpu.get_barrier_semaphore()
    for k in range(1, tp_count):
        pl.semaphore_signal(
            barrier, inc=1, device_id=(ep_at, lax.rem(tp_at + k, tp_count)), device_id_type=MESH
        )
    for k in range(1, ep_count):
        pl.semaphore_signal(
            barrier, inc=1, device_id=(lax.rem(ep_at + k, ep_count), tp_at), device_id_type=MESH
        )

    residual_in = tokens[...].astype(F32)
    normed = normalized(residual_in, mix_gain[...])

    def eye(n):
        return lax.broadcasted_iota(jnp.int32, (n, n), 0) == lax.broadcasted_iota(
            jnp.int32, (n, n), 1
        )

    def column(row):
        return jnp.sum(jnp.where(eye(seqs), row, jnp.zeros_like(row)), axis=1, keepdims=True)

    def row_of(col):
        return jnp.sum(jnp.where(eye(seqs), col, jnp.zeros_like(col)), axis=0, keepdims=True)

    contract = (((1,), (1,)), ((), ()))
    gates_i = lax.dot_general(normed, igate_rows[...], contract, preferred_element_type=F32)
    gates_f = lax.dot_general(normed, fgate_rows[...], contract, preferred_element_type=F32)
    lane = lax.broadcasted_iota(jnp.int32, gates_i.shape, 1)

    def slot_masks(shape, dim, group):
        at = lax.broadcasted_iota(jnp.int32, shape, dim)
        return at // group // slots, at % slots

    id0, id1 = ids[0:1, :], ids[1:2, :]
    expert_r, slot_r = slot_masks((experts * slots, seqs), 0, 1)
    match_r = jnp.where((id0 == expert_r) | (id1 == expert_r), 1.0, 0.0)
    before = lax.broadcasted_iota(jnp.int32, (seqs, seqs), 0) < lax.broadcasted_iota(
        jnp.int32, (seqs, seqs), 1
    )
    rank_r = jnp.dot(match_r, jnp.where(before, 1.0, 0.0), preferred_element_type=F32)
    placing = jnp.where(rank_r == slot_r.astype(F32), match_r, 0.0).astype(BF16)
    id0c, id1c = column(id0), column(id1)
    w0c, w1c = column(route_w[0:1, :]), column(route_w[1:2, :])
    at_c = lax.broadcasted_iota(jnp.int32, (seqs, ep_count * slots), 1)
    expert_c, slot_c = at_c // (slots * span), at_c % slots
    first, second = id0c == expert_c, id1c == expert_c
    match_c = jnp.where(first | second, 1.0, 0.0)
    after = lax.broadcasted_iota(jnp.int32, (seqs, seqs), 0) > lax.broadcasted_iota(
        jnp.int32, (seqs, seqs), 1
    )
    rank_c = jnp.dot(jnp.where(after, 1.0, 0.0), match_c, preferred_element_type=F32)
    mixing = jnp.where(
        rank_c == slot_c.astype(F32),
        jnp.where(first, w0c, 0.0) + jnp.where(second, w1c, 0.0),
        0.0,
    )

    for copy in loads:
        copy.wait()
    projected = [
        jnp.dot(normed, qkv_buf[i], preferred_element_type=F32).astype(BF16).astype(F32)
        for i in range(3)
    ]
    load_mem.wait()
    readouts, maxes = [], []
    for h in range(heads):
        at = tp_at * heads + h
        cut = slice(h * head_dim, (h + 1) * head_dim)
        query, value = projected[0][:, cut], projected[2][:, cut]
        key = projected[1][:, cut] * head_dim ** (-0.5)
        input_gate = jnp.sum(jnp.where(lane == at, gates_i, 0.0), axis=1, keepdims=True)
        pre = jnp.sum(jnp.where(lane == at, gates_f, 0.0), axis=1, keepdims=True) + forget_bias[at]
        forget_log = jnp.minimum(pre, 0.0) - jnp.log1p(jnp.exp(-jnp.abs(pre)))
        held = forget_log + column(max_row[h : h + 1, :])
        top = jnp.maximum(held, input_gate)
        keep = jnp.exp(held - top)
        fresh = jnp.exp(input_gate - top)
        new_max_row[h : h + 1, :] = row_of(top)
        norm = keep * norm_state[:, cut] + fresh * key
        new_norm[:, cut] = norm
        under = jnp.sum(query * norm, axis=1, keepdims=True)
        scaled = fresh * key
        pad = jnp.zeros((head_dim - 2 * seqs, head_dim), F32)
        turned = jnp.transpose(jnp.concatenate([scaled, query, pad], axis=0))
        over = []
        for s in range(seqs):
            cell = keep[s : s + 1, :] * mem_buf[s, h] + turned[:, s : s + 1] * value[s : s + 1, :]
            mem_buf[s, h] = cell
            over.append(jnp.sum(turned[:, seqs + s : seqs + s + 1] * cell, axis=0, keepdims=True))
        over = jnp.concatenate(over, axis=0)
        readouts.append((over / jnp.maximum(jnp.abs(under), jnp.exp(-top))).astype(BF16))
    readout = readouts[0] if heads == 1 else jnp.concatenate(readouts, axis=1)
    load_out.wait()
    parts[tp_at] = jnp.dot(readout, out_buf[...], preferred_element_type=F32).astype(BF16)
    pl.semaphore_wait(barrier, tp_count - 1 + ep_count - 1)

    def send(src, dst, sems, recvs, k, device):
        copy = pltpu.make_async_remote_copy(
            src_ref=src,
            dst_ref=dst,
            send_sem=sems.at[k],
            recv_sem=recvs.at[k],
            device_id=device,
            device_id_type=MESH,
        )
        copy.start()
        return copy

    sent = []
    part_copies = [
        send(
            parts.at[tp_at],
            parts.at[tp_at],
            part_send,
            part_recv,
            k,
            (ep_at, lax.rem(tp_at + k, tp_count)),
        )
        for k in range(1, tp_count)
    ]
    store_mem = pltpu.make_async_copy(mem_buf, new_memory, mem_sem)
    store_mem.start()
    for copy in part_copies:
        copy.wait_recv()
    sent += part_copies
    head_total = parts[0].astype(F32)
    for t in range(1, tp_count):
        head_total = head_total + parts[t].astype(F32)
    residual = (residual_in + head_total).astype(BF16).astype(F32)
    residual_buf[...] = residual
    outgoing = normalized(residual, ffn_gain[...])
    rows = jnp.dot(placing, outgoing, preferred_element_type=F32)
    for e in range(experts):
        packed[e] = rows[e * slots : (e + 1) * slots, :].astype(BF16)
    row_copies = []
    for k in range(1, ep_count):
        to = lax.rem(ep_at + k, ep_count)
        row_copies.append(
            send(packed.at[to // span], arrived.at[ep_at], row_send, row_recv, k, (to, tp_at))
        )
    arrived[ep_at] = packed[ep_at // span]
    load_gate.wait()
    load_up.wait()
    for copy in row_copies:
        copy.wait_recv()
    sent += row_copies
    flat = merged(arrived, ep_count).astype(BF16)
    units = gate_buf.shape[1]
    step = min(256, units)
    for at in range(0, units, step):
        gate = jnp.dot(flat, gate_buf[:, at : at + step], preferred_element_type=F32)
        up = jnp.dot(flat, up_buf[:, at : at + step], preferred_element_type=F32)
        hidden_all[tp_at, :, at : at + step] = (gate * jax.nn.sigmoid(gate) * up).astype(BF16)
    hid_copies = [
        send(
            hidden_all.at[tp_at],
            hidden_all.at[tp_at],
            hid_send,
            hid_recv,
            k,
            (ep_at, lax.rem(tp_at + k, tp_count)),
        )
        for k in range(1, tp_count)
    ]
    load_down.wait()
    total = None
    for k in range(tp_count):
        if k:
            hid_copies[k - 1].wait_recv()
        source = lax.rem(tp_at - k + tp_count, tp_count)
        start = pl.multiple_of(source * units, units)
        term = jnp.dot(
            hidden_all[source], down_buf[pl.ds(start, units), :], preferred_element_type=F32
        )
        total = term if total is None else total + term
    sent += hid_copies
    for i in range(ep_count):
        back[i] = total[i * slots : (i + 1) * slots, :].astype(BF16)
    back_copies = []
    for k in range(1, ep_count):
        to = lax.rem(ep_at + k, ep_count)
        back_copies.append(
            send(back.at[to], returned.at[ep_at], back_send, back_recv, k, (to, tp_at))
        )
    returned[ep_at] = back[ep_at]
    for copy in back_copies:
        copy.wait_recv()
    sent += back_copies
    results = merged(returned, ep_count)
    routed = jnp.dot(
        mixing, results, precision=lax.Precision.HIGHEST, preferred_element_type=F32
    )
    own = residual_buf[:, pl.ds(pl.multiple_of(tp_at * own_width, own_width), own_width)]
    out_tokens[...] = (own + routed).astype(BF16)
    for copy in sent:
        copy.wait_send()
    store_mem.wait()


def shards(
    tokens,
    mix_gain,
    w_query,
    w_key,
    w_value,
    w_igate,
    w_fgate,
    forget_bias,
    w_out,
    mem_state,
    norm_state,
    max_state,
    ffn_gain,
    route_ids,
    route_weights,
    w_gate,
    w_up,
    w_down,
):
    seqs, width = tokens.shape
    heads = mem_state.shape[1]
    head_dim = norm_state.shape[1] // heads
    tp_count = lax.axis_size("tp")
    ep_count = lax.axis_size("ep")
    own_width = width // tp_count
    top_count = route_ids.shape[1]
    span = FF // w_down.shape[0]
    experts = ep_count // span
    slot_cap = max(2, 3 * seqs * top_count // (2 * experts))
    slots = -(-slot_cap // 4) * 4
    memory = mem_state.reshape(seqs, heads, head_dim, head_dim)
    total = ep_count * slots
    units = w_gate.shape[1]
    vmem = pl.BlockSpec(memory_space=pltpu.VMEM)
    smem = pl.BlockSpec(memory_space=pltpu.SMEM)
    hbm = pl.BlockSpec(memory_space=pl.ANY)
    dma = pltpu.SemaphoreType.DMA
    outs = pl.pallas_call(
        functools.partial(kernel, (tp_count, ep_count, span, experts, slots, heads)),
        out_shape=(
            jax.ShapeDtypeStruct((seqs, own_width), BF16),
            jax.ShapeDtypeStruct(memory.shape, F32),
            jax.ShapeDtypeStruct(norm_state.shape, F32),
            jax.ShapeDtypeStruct((heads, seqs), F32),
        ),
        in_specs=[vmem] * 4 + [smem] + [vmem] * 5 + [hbm] * 8,
        out_specs=(vmem, hbm, vmem, vmem),
        scratch_shapes=[
            pltpu.VMEM((3,) + w_query.shape, BF16),
            pltpu.VMEM(w_out.shape, BF16),
            pltpu.VMEM(memory.shape, F32),
            pltpu.VMEM(w_gate.shape, BF16),
            pltpu.VMEM(w_up.shape, BF16),
            pltpu.VMEM(w_down.shape, BF16),
            pltpu.VMEM((tp_count, seqs, width), BF16),
            pltpu.VMEM((seqs, width), F32),
            pltpu.VMEM((experts, slots, width), BF16),
            pltpu.VMEM((ep_count, slots, width), BF16),
            pltpu.VMEM((tp_count, total, units), BF16),
            pltpu.VMEM((ep_count, slots, own_width), BF16),
            pltpu.VMEM((ep_count, slots, own_width), BF16),
            dma((8,)),
            dma,
            dma((tp_count,)),
            dma((tp_count,)),
            dma((ep_count,)),
            dma((ep_count,)),
            dma((tp_count,)),
            dma((tp_count,)),
            dma((ep_count,)),
            dma((ep_count,)),
        ],
        compiler_params=pltpu.CompilerParams(
            collective_id=0, has_side_effects=True, vmem_limit_bytes=60 * 1024 * 1024
        ),
    )(
        tokens,
        mix_gain.astype(F32).reshape(1, width),
        w_igate.T,
        w_fgate.T,
        forget_bias,
        norm_state,
        max_state.T,
        ffn_gain.astype(F32).reshape(1, width),
        route_ids.T,
        route_weights.T,
        w_query,
        w_key,
        w_value,
        w_out,
        memory,
        w_gate,
        w_up,
        w_down,
    )
    return outs[0], outs[1].reshape(mem_state.shape), outs[2], outs[3].T


def solution(mesh):
    placed = (
        P("ep", None),
        P(),
        P(None, "tp"),
        P(None, "tp"),
        P(None, "tp"),
        P(),
        P(),
        P(),
        P("tp", None),
        P("ep", "tp", None),
        P("ep", "tp"),
        P("ep", "tp"),
        P(),
        P("ep", None),
        P("ep", None),
        P(None, ("ep", "tp")),
        P(None, ("ep", "tp")),
        P("ep", "tp"),
    )
    return jax.shard_map(
        shards,
        mesh=mesh,
        in_specs=placed,
        out_specs=(P("ep", "tp"), P("ep", "tp", None), P("ep", "tp"), P("ep", "tp")),
        check_vma=False,
    )
```

```python
import functools

import jax
import jax.numpy as jnp
from jax import lax
from jax.experimental import pallas as pl
from jax.experimental.pallas import tpu as pltpu
from jax.sharding import PartitionSpec as P

FF = 4096
epsilon = 1e-06
MESH = pl.DeviceIdType.MESH
F32 = jnp.float32
BF16 = jnp.bfloat16


def normalized(rows, gain):
    squares = jnp.sum(rows * rows, axis=1, keepdims=True) / rows.shape[1]
    return (rows * lax.rsqrt(squares + epsilon) * gain).astype(BF16)


def merged(ref, count):
    return jnp.concatenate([ref[i].astype(F32) for i in range(count)], axis=0)


def kernel(
    sizes,
    tokens,
    mix_gain,
    igate_rows,
    fgate_rows,
    forget_bias,
    norm_state,
    max_row,
    ffn_gain,
    ids,
    route_w,
    w_query,
    w_key,
    w_value,
    w_out,
    mem_state,
    w_gate,
    w_up,
    w_down,
    out_tokens,
    new_memory,
    new_norm,
    new_max_row,
    qkv_buf,
    out_buf,
    mem_buf,
    gate_buf,
    up_buf,
    down_buf,
    parts,
    residual_buf,
    packed,
    arrived,
    hidden_all,
    back,
    returned,
    load_sem,
    mem_sem,
    part_send,
    part_recv,
    row_send,
    row_recv,
    hid_send,
    hid_recv,
    back_send,
    back_recv,
):
    tp_count, ep_count, span, experts, slots, heads = sizes
    tp_at = lax.axis_index("tp")
    ep_at = lax.axis_index("ep")
    seqs, width = tokens.shape
    head_dim = mem_buf.shape[-1]
    own_width = out_tokens.shape[1]

    def load(src, dst, at):
        copy = pltpu.make_async_copy(src, dst, load_sem.at[at])
        copy.start()
        return copy

    loads = [load(w, qkv_buf.at[i], i) for i, w in enumerate((w_query, w_key, w_value))]
    load_mem = load(mem_state, mem_buf, 3)
    load_out = load(w_out, out_buf, 4)
    load_gate = load(w_gate, gate_buf, 5)
    load_up = load(w_up, up_buf, 6)
    load_down = load(w_down, down_buf, 7)

    barrier = pltpu.get_barrier_semaphore()
    for k in range(1, tp_count):
        pl.semaphore_signal(
            barrier, inc=1, device_id=(ep_at, lax.rem(tp_at + k, tp_count)), device_id_type=MESH
        )
    for k in range(1, ep_count):
        pl.semaphore_signal(
            barrier, inc=1, device_id=(lax.rem(ep_at + k, ep_count), tp_at), device_id_type=MESH
        )

    residual_in = tokens[...].astype(F32)
    normed = normalized(residual_in, mix_gain[...].astype(F32).reshape(1, width))

    def eye(n):
        return lax.broadcasted_iota(jnp.int32, (n, n), 0) == lax.broadcasted_iota(
            jnp.int32, (n, n), 1
        )

    def column(row):
        return jnp.sum(jnp.where(eye(seqs), row, jnp.zeros_like(row)), axis=1, keepdims=True)

    def row_of(col):
        return jnp.sum(jnp.where(eye(seqs), col, jnp.zeros_like(col)), axis=0, keepdims=True)

    contract = (((1,), (1,)), ((), ()))
    gates_i = lax.dot_general(normed, igate_rows[...], contract, preferred_element_type=F32)
    gates_f = lax.dot_general(normed, fgate_rows[...], contract, preferred_element_type=F32)
    lane = lax.broadcasted_iota(jnp.int32, gates_i.shape, 1)

    def slot_masks(shape, dim, group):
        at = lax.broadcasted_iota(jnp.int32, shape, dim)
        return at // group // slots, at % slots

    id0, id1 = ids[0:1, :], ids[1:2, :]
    expert_r, slot_r = slot_masks((experts * slots, seqs), 0, 1)
    match_r = jnp.where((id0 == expert_r) | (id1 == expert_r), 1.0, 0.0)
    before = lax.broadcasted_iota(jnp.int32, (seqs, seqs), 0) < lax.broadcasted_iota(
        jnp.int32, (seqs, seqs), 1
    )
    rank_r = jnp.dot(match_r, jnp.where(before, 1.0, 0.0), preferred_element_type=F32)
    placing = jnp.where(rank_r == slot_r.astype(F32), match_r, 0.0).astype(BF16)
    id0c, id1c = column(id0), column(id1)
    w0c, w1c = column(route_w[0:1, :]), column(route_w[1:2, :])
    at_c = lax.broadcasted_iota(jnp.int32, (seqs, ep_count * slots), 1)
    expert_c, slot_c = at_c // (slots * span), at_c % slots
    first, second = id0c == expert_c, id1c == expert_c
    match_c = jnp.where(first | second, 1.0, 0.0)
    after = lax.broadcasted_iota(jnp.int32, (seqs, seqs), 0) > lax.broadcasted_iota(
        jnp.int32, (seqs, seqs), 1
    )
    rank_c = jnp.dot(jnp.where(after, 1.0, 0.0), match_c, preferred_element_type=F32)
    mixing = jnp.where(
        rank_c == slot_c.astype(F32),
        jnp.where(first, w0c, 0.0) + jnp.where(second, w1c, 0.0),
        0.0,
    )

    for copy in loads:
        copy.wait()
    projected = [
        jnp.dot(normed, qkv_buf[i], preferred_element_type=F32).astype(BF16).astype(F32)
        for i in range(3)
    ]
    load_mem.wait()
    readouts, maxes = [], []
    for h in range(heads):
        at = tp_at * heads + h
        cut = slice(h * head_dim, (h + 1) * head_dim)
        query, value = projected[0][:, cut], projected[2][:, cut]
        key = projected[1][:, cut] * head_dim ** (-0.5)
        input_gate = jnp.sum(jnp.where(lane == at, gates_i, 0.0), axis=1, keepdims=True)
        pre = jnp.sum(jnp.where(lane == at, gates_f, 0.0), axis=1, keepdims=True) + forget_bias[at]
        forget_log = jnp.minimum(pre, 0.0) - jnp.log1p(jnp.exp(-jnp.abs(pre)))
        held = forget_log + column(max_row[h : h + 1, :])
        top = jnp.maximum(held, input_gate)
        keep = jnp.exp(held - top)
        fresh = jnp.exp(input_gate - top)
        new_max_row[h : h + 1, :] = row_of(top)
        norm = keep * norm_state[:, cut] + fresh * key
        new_norm[:, cut] = norm
        under = jnp.sum(query * norm, axis=1, keepdims=True)
        scaled = fresh * key
        pad = jnp.zeros((head_dim - 2 * seqs, head_dim), F32)
        turned = jnp.transpose(jnp.concatenate([scaled, query, pad], axis=0))
        over = []
        for s in range(seqs):
            cell = keep[s : s + 1, :] * mem_buf[s, h] + turned[:, s : s + 1] * value[s : s + 1, :]
            mem_buf[s, h] = cell
            over.append(jnp.sum(turned[:, seqs + s : seqs + s + 1] * cell, axis=0, keepdims=True))
        over = jnp.concatenate(over, axis=0)
        readouts.append((over / jnp.maximum(jnp.abs(under), jnp.exp(-top))).astype(BF16))
    readout = readouts[0] if heads == 1 else jnp.concatenate(readouts, axis=1)
    load_out.wait()
    parts[tp_at] = jnp.dot(readout, out_buf[...], preferred_element_type=F32).astype(BF16)
    pl.semaphore_wait(barrier, tp_count - 1 + ep_count - 1)

    def send(src, dst, sems, recvs, k, device):
        copy = pltpu.make_async_remote_copy(
            src_ref=src,
            dst_ref=dst,
            send_sem=sems.at[k],
            recv_sem=recvs.at[k],
            device_id=device,
            device_id_type=MESH,
        )
        copy.start()
        return copy

    sent = []
    part_copies = [
        send(
            parts.at[tp_at],
            parts.at[tp_at],
            part_send,
            part_recv,
            k,
            (ep_at, lax.rem(tp_at + k, tp_count)),
        )
        for k in range(1, tp_count)
    ]
    store_mem = pltpu.make_async_copy(mem_buf, new_memory, mem_sem)
    store_mem.start()
    for copy in part_copies:
        copy.wait_recv()
    sent += part_copies
    head_total = parts[0].astype(F32)
    for t in range(1, tp_count):
        head_total = head_total + parts[t].astype(F32)
    residual = (residual_in + head_total).astype(BF16).astype(F32)
    residual_buf[...] = residual
    outgoing = normalized(residual, ffn_gain[...].astype(F32).reshape(1, width))
    rows = jnp.dot(placing, outgoing, preferred_element_type=F32)
    for e in range(experts):
        packed[e] = rows[e * slots : (e + 1) * slots, :].astype(BF16)
    row_copies = []
    for k in range(1, ep_count):
        to = lax.rem(ep_at + k, ep_count)
        row_copies.append(
            send(packed.at[to // span], arrived.at[ep_at], row_send, row_recv, k, (to, tp_at))
        )
    arrived[ep_at] = packed[ep_at // span]
    load_gate.wait()
    load_up.wait()
    for copy in row_copies:
        copy.wait_recv()
    sent += row_copies
    flat = merged(arrived, ep_count).astype(BF16)
    units = gate_buf.shape[1]
    step = min(256, units)
    for at in range(0, units, step):
        gate = jnp.dot(flat, gate_buf[:, at : at + step], preferred_element_type=F32)
        up = jnp.dot(flat, up_buf[:, at : at + step], preferred_element_type=F32)
        hidden_all[tp_at, :, at : at + step] = (gate * jax.nn.sigmoid(gate) * up).astype(BF16)
    hid_copies = [
        send(
            hidden_all.at[tp_at],
            hidden_all.at[tp_at],
            hid_send,
            hid_recv,
            k,
            (ep_at, lax.rem(tp_at + k, tp_count)),
        )
        for k in range(1, tp_count)
    ]
    load_down.wait()
    total = None
    for k in range(tp_count):
        if k:
            hid_copies[k - 1].wait_recv()
        source = lax.rem(tp_at - k + tp_count, tp_count)
        start = pl.multiple_of(source * units, units)
        term = jnp.dot(
            hidden_all[source], down_buf[pl.ds(start, units), :], preferred_element_type=F32
        )
        total = term if total is None else total + term
    sent += hid_copies
    for i in range(ep_count):
        back[i] = total[i * slots : (i + 1) * slots, :].astype(BF16)
    back_copies = []
    for k in range(1, ep_count):
        to = lax.rem(ep_at + k, ep_count)
        back_copies.append(
            send(back.at[to], returned.at[ep_at], back_send, back_recv, k, (to, tp_at))
        )
    returned[ep_at] = back[ep_at]
    for copy in back_copies:
        copy.wait_recv()
    sent += back_copies
    results = merged(returned, ep_count)
    routed = jnp.dot(
        mixing, results, precision=lax.Precision.HIGHEST, preferred_element_type=F32
    )
    own = residual_buf[:, pl.ds(pl.multiple_of(tp_at * own_width, own_width), own_width)]
    out_tokens[...] = (own + routed).astype(BF16)
    for copy in sent:
        copy.wait_send()
    store_mem.wait()


def hand_on(count, *refs):
    sources, targets, held = refs[:count], refs[count : 2 * count], refs[2 * count : 3 * count]
    in_sem, out_sem = refs[3 * count :]
    reads = [
        pltpu.make_async_copy(sources[i], held[i], in_sem.at[i]) for i in range(count)
    ]
    writes = [
        pltpu.make_async_copy(held[i], targets[i], out_sem.at[i]) for i in range(count)
    ]
    for copy in reads:
        copy.start()
    for read, write in zip(reads, writes):
        read.wait()
        write.start()
    for copy in writes:
        copy.wait()


def shards(
    tokens,
    mix_gain,
    w_query,
    w_key,
    w_value,
    w_igate,
    w_fgate,
    forget_bias,
    w_out,
    mem_state,
    norm_state,
    max_state,
    ffn_gain,
    route_ids,
    route_weights,
    w_gate,
    w_up,
    w_down,
):
    seqs, width = tokens.shape
    heads = mem_state.shape[1]
    head_dim = norm_state.shape[1] // heads
    tp_count = lax.axis_size("tp")
    ep_count = lax.axis_size("ep")
    own_width = width // tp_count
    top_count = route_ids.shape[1]
    span = FF // w_down.shape[0]
    experts = ep_count // span
    slot_cap = max(2, 3 * seqs * top_count // (2 * experts))
    slots = -(-slot_cap // 4) * 4
    memory = mem_state.reshape(seqs, heads, head_dim, head_dim)
    total = ep_count * slots
    units = w_gate.shape[1]
    vmem = pl.BlockSpec(memory_space=pltpu.VMEM)
    smem = pl.BlockSpec(memory_space=pltpu.SMEM)
    hbm = pl.BlockSpec(memory_space=pl.ANY)
    dma = pltpu.SemaphoreType.DMA
    outs = pl.pallas_call(
        functools.partial(kernel, (tp_count, ep_count, span, experts, slots, heads)),
        out_shape=(
            jax.ShapeDtypeStruct((seqs, own_width), BF16),
            jax.ShapeDtypeStruct(memory.shape, F32),
            jax.ShapeDtypeStruct(norm_state.shape, F32),
            jax.ShapeDtypeStruct((heads, seqs), F32),
        ),
        in_specs=[vmem] * 4 + [smem] + [vmem] * 5 + [hbm] * 8,
        out_specs=(vmem, hbm, vmem, vmem),
        scratch_shapes=[
            pltpu.VMEM((3,) + w_query.shape, BF16),
            pltpu.VMEM(w_out.shape, BF16),
            pltpu.VMEM(memory.shape, F32),
            pltpu.VMEM(w_gate.shape, BF16),
            pltpu.VMEM(w_up.shape, BF16),
            pltpu.VMEM(w_down.shape, BF16),
            pltpu.VMEM((tp_count, seqs, width), BF16),
            pltpu.VMEM((seqs, width), F32),
            pltpu.VMEM((experts, slots, width), BF16),
            pltpu.VMEM((ep_count, slots, width), BF16),
            pltpu.VMEM((tp_count, total, units), BF16),
            pltpu.VMEM((ep_count, slots, own_width), BF16),
            pltpu.VMEM((ep_count, slots, own_width), BF16),
            dma((8,)),
            dma,
            dma((tp_count,)),
            dma((tp_count,)),
            dma((ep_count,)),
            dma((ep_count,)),
            dma((tp_count,)),
            dma((tp_count,)),
            dma((ep_count,)),
            dma((ep_count,)),
        ],
        compiler_params=pltpu.CompilerParams(
            collective_id=0, has_side_effects=True, vmem_limit_bytes=60 * 1024 * 1024
        ),
    )(
        tokens,
        mix_gain,
        w_igate.T,
        w_fgate.T,
        forget_bias,
        norm_state,
        max_state.T,
        ffn_gain,
        route_ids.T,
        route_weights.T,
        w_query,
        w_key,
        w_value,
        w_out,
        memory,
        w_gate,
        w_up,
        w_down,
    )
    outs = pl.pallas_call(
        functools.partial(hand_on, len(outs)),
        out_shape=tuple(jax.ShapeDtypeStruct(o.shape, o.dtype) for o in outs),
        in_specs=[hbm] * len(outs),
        out_specs=(hbm,) * len(outs),
        scratch_shapes=[pltpu.VMEM(o.shape, o.dtype) for o in outs]
        + [dma((len(outs),)), dma((len(outs),))],
        compiler_params=pltpu.CompilerParams(vmem_limit_bytes=60 * 1024 * 1024),
    )(*outs)
    return outs[0], outs[1].reshape(mem_state.shape), outs[2], outs[3].T


def solution(mesh):
    placed = (
        P("ep", None),
        P(),
        P(None, "tp"),
        P(None, "tp"),
        P(None, "tp"),
        P(),
        P(),
        P(),
        P("tp", None),
        P("ep", "tp", None),
        P("ep", "tp"),
        P("ep", "tp"),
        P(),
        P("ep", None),
        P("ep", None),
        P(None, ("ep", "tp")),
        P(None, ("ep", "tp")),
        P("ep", "tp"),
    )
    return jax.shard_map(
        shards,
        mesh=mesh,
        in_specs=placed,
        out_specs=(P("ep", "tp"), P("ep", "tp", None), P("ep", "tp"), P("ep", "tp")),
        check_vma=False,
    )
```

```python
import functools

import jax
import jax.numpy as jnp
from jax import lax
from jax.experimental import pallas as pl
from jax.experimental.pallas import tpu as pltpu
from jax.sharding import PartitionSpec as P

FF = 4096
epsilon = 1e-06
MESH = pl.DeviceIdType.MESH
F32 = jnp.float32
BF16 = jnp.bfloat16


def normalized(rows, gain):
    squares = jnp.sum(rows * rows, axis=1, keepdims=True) / rows.shape[1]
    return (rows * lax.rsqrt(squares + epsilon) * gain).astype(BF16)


def merged(ref, count):
    return jnp.concatenate([ref[i].astype(F32) for i in range(count)], axis=0)


def kernel(
    sizes,
    tokens,
    mix_gain,
    igate_rows,
    fgate_rows,
    forget_bias,
    norm_state,
    max_row,
    ffn_gain,
    ids,
    route_w,
    w_query,
    w_key,
    w_value,
    w_out,
    mem_state,
    w_gate,
    w_up,
    w_down,
    out_tokens,
    new_memory,
    new_norm,
    new_max_row,
    qkv_buf,
    out_buf,
    gate_buf,
    up_buf,
    down_buf,
    parts,
    residual_buf,
    packed,
    arrived,
    hidden_all,
    back,
    returned,
    load_sem,
    part_send,
    part_recv,
    row_send,
    row_recv,
    hid_send,
    hid_recv,
    back_send,
    back_recv,
):
    tp_count, ep_count, span, experts, slots, heads = sizes
    tp_at = lax.axis_index("tp")
    ep_at = lax.axis_index("ep")
    seqs, width = tokens.shape
    head_dim = new_memory.shape[-1]
    own_width = out_tokens.shape[1]

    def load(src, dst, at):
        copy = pltpu.make_async_copy(src, dst, load_sem.at[at])
        copy.start()
        return copy

    loads = [load(w, qkv_buf.at[i], i) for i, w in enumerate((w_query, w_key, w_value))]
    load_mem = load(mem_state, new_memory, 3)
    load_out = load(w_out, out_buf, 4)
    load_gate = load(w_gate, gate_buf, 5)
    load_up = load(w_up, up_buf, 6)
    load_down = load(w_down, down_buf, 7)

    barrier = pltpu.get_barrier_semaphore()
    for k in range(1, tp_count):
        pl.semaphore_signal(
            barrier, inc=1, device_id=(ep_at, lax.rem(tp_at + k, tp_count)), device_id_type=MESH
        )
    for k in range(1, ep_count):
        pl.semaphore_signal(
            barrier, inc=1, device_id=(lax.rem(ep_at + k, ep_count), tp_at), device_id_type=MESH
        )

    residual_in = tokens[...].astype(F32)
    normed = normalized(residual_in, mix_gain[...].astype(F32).reshape(1, width))

    def eye(n):
        return lax.broadcasted_iota(jnp.int32, (n, n), 0) == lax.broadcasted_iota(
            jnp.int32, (n, n), 1
        )

    def column(row):
        return jnp.sum(jnp.where(eye(seqs), row, jnp.zeros_like(row)), axis=1, keepdims=True)

    def row_of(col):
        return jnp.sum(jnp.where(eye(seqs), col, jnp.zeros_like(col)), axis=0, keepdims=True)

    contract = (((1,), (1,)), ((), ()))
    gates_i = lax.dot_general(normed, igate_rows[...], contract, preferred_element_type=F32)
    gates_f = lax.dot_general(normed, fgate_rows[...], contract, preferred_element_type=F32)
    lane = lax.broadcasted_iota(jnp.int32, gates_i.shape, 1)

    def slot_masks(shape, dim, group):
        at = lax.broadcasted_iota(jnp.int32, shape, dim)
        return at // group // slots, at % slots

    id0, id1 = ids[0:1, :], ids[1:2, :]
    expert_r, slot_r = slot_masks((experts * slots, seqs), 0, 1)
    match_r = jnp.where((id0 == expert_r) | (id1 == expert_r), 1.0, 0.0)
    before = lax.broadcasted_iota(jnp.int32, (seqs, seqs), 0) < lax.broadcasted_iota(
        jnp.int32, (seqs, seqs), 1
    )
    rank_r = jnp.dot(match_r, jnp.where(before, 1.0, 0.0), preferred_element_type=F32)
    placing = jnp.where(rank_r == slot_r.astype(F32), match_r, 0.0).astype(BF16)
    id0c, id1c = column(id0), column(id1)
    w0c, w1c = column(route_w[0:1, :]), column(route_w[1:2, :])
    at_c = lax.broadcasted_iota(jnp.int32, (seqs, ep_count * slots), 1)
    expert_c, slot_c = at_c // (slots * span), at_c % slots
    first, second = id0c == expert_c, id1c == expert_c
    match_c = jnp.where(first | second, 1.0, 0.0)
    after = lax.broadcasted_iota(jnp.int32, (seqs, seqs), 0) > lax.broadcasted_iota(
        jnp.int32, (seqs, seqs), 1
    )
    rank_c = jnp.dot(jnp.where(after, 1.0, 0.0), match_c, preferred_element_type=F32)
    mixing = jnp.where(
        rank_c == slot_c.astype(F32),
        jnp.where(first, w0c, 0.0) + jnp.where(second, w1c, 0.0),
        0.0,
    )

    for copy in loads:
        copy.wait()
    projected = [
        jnp.dot(normed, qkv_buf[i], preferred_element_type=F32).astype(BF16).astype(F32)
        for i in range(3)
    ]
    load_mem.wait()
    readouts, maxes = [], []
    for h in range(heads):
        at = tp_at * heads + h
        cut = slice(h * head_dim, (h + 1) * head_dim)
        query, value = projected[0][:, cut], projected[2][:, cut]
        key = projected[1][:, cut] * head_dim ** (-0.5)
        input_gate = jnp.sum(jnp.where(lane == at, gates_i, 0.0), axis=1, keepdims=True)
        pre = jnp.sum(jnp.where(lane == at, gates_f, 0.0), axis=1, keepdims=True) + forget_bias[at]
        forget_log = jnp.minimum(pre, 0.0) - jnp.log1p(jnp.exp(-jnp.abs(pre)))
        held = forget_log + column(max_row[h : h + 1, :])
        top = jnp.maximum(held, input_gate)
        keep = jnp.exp(held - top)
        fresh = jnp.exp(input_gate - top)
        new_max_row[h : h + 1, :] = row_of(top)
        norm = keep * norm_state[:, cut] + fresh * key
        new_norm[:, cut] = norm
        under = jnp.sum(query * norm, axis=1, keepdims=True)
        scaled = fresh * key
        pad = jnp.zeros((head_dim - 2 * seqs, head_dim), F32)
        turned = jnp.transpose(jnp.concatenate([scaled, query, pad], axis=0))
        over = []
        for s in range(seqs):
            cell = keep[s : s + 1, :] * new_memory[s, h] + turned[:, s : s + 1] * value[s : s + 1, :]
            new_memory[s, h] = cell
            over.append(jnp.sum(turned[:, seqs + s : seqs + s + 1] * cell, axis=0, keepdims=True))
        over = jnp.concatenate(over, axis=0)
        readouts.append((over / jnp.maximum(jnp.abs(under), jnp.exp(-top))).astype(BF16))
    readout = readouts[0] if heads == 1 else jnp.concatenate(readouts, axis=1)
    load_out.wait()
    parts[tp_at] = jnp.dot(readout, out_buf[...], preferred_element_type=F32).astype(BF16)
    pl.semaphore_wait(barrier, tp_count - 1 + ep_count - 1)

    def send(src, dst, sems, recvs, k, device):
        copy = pltpu.make_async_remote_copy(
            src_ref=src,
            dst_ref=dst,
            send_sem=sems.at[k],
            recv_sem=recvs.at[k],
            device_id=device,
            device_id_type=MESH,
        )
        copy.start()
        return copy

    sent = []
    part_copies = [
        send(
            parts.at[tp_at],
            parts.at[tp_at],
            part_send,
            part_recv,
            k,
            (ep_at, lax.rem(tp_at + k, tp_count)),
        )
        for k in range(1, tp_count)
    ]
    for copy in part_copies:
        copy.wait_recv()
    sent += part_copies
    head_total = parts[0].astype(F32)
    for t in range(1, tp_count):
        head_total = head_total + parts[t].astype(F32)
    residual = (residual_in + head_total).astype(BF16).astype(F32)
    residual_buf[...] = residual
    outgoing = normalized(residual, ffn_gain[...].astype(F32).reshape(1, width))
    rows = jnp.dot(placing, outgoing, preferred_element_type=F32)
    for e in range(experts):
        packed[e] = rows[e * slots : (e + 1) * slots, :].astype(BF16)
    row_copies = []
    for k in range(1, ep_count):
        to = lax.rem(ep_at + k, ep_count)
        row_copies.append(
            send(packed.at[to // span], arrived.at[ep_at], row_send, row_recv, k, (to, tp_at))
        )
    arrived[ep_at] = packed[ep_at // span]
    load_gate.wait()
    load_up.wait()
    for copy in row_copies:
        copy.wait_recv()
    sent += row_copies
    flat = merged(arrived, ep_count).astype(BF16)
    units = gate_buf.shape[1]
    chunks, step = hidden_all.shape[1], hidden_all.shape[3]
    hid_copies = {}
    for c in range(chunks):
        cut = slice(c * step, (c + 1) * step)
        gate = jnp.dot(flat, gate_buf[:, cut], preferred_element_type=F32)
        up = jnp.dot(flat, up_buf[:, cut], preferred_element_type=F32)
        hidden_all[tp_at, c] = (gate * jax.nn.sigmoid(gate) * up).astype(BF16)
        for k in range(1, tp_count):
            hid_copies[k, c] = send(
                hidden_all.at[tp_at, c],
                hidden_all.at[tp_at, c],
                hid_send,
                hid_recv,
                k * chunks + c,
                (ep_at, lax.rem(tp_at + k, tp_count)),
            )
    load_down.wait()
    total = None
    for k, c in [(0, c) for c in range(chunks)] + [
        (k, c) for c in range(chunks) for k in range(1, tp_count)
    ]:
        if k:
            hid_copies[k, c].wait_recv()
        source = lax.rem(tp_at - k + tp_count, tp_count)
        start = pl.multiple_of(source * units + c * step, step)
        term = jnp.dot(
            hidden_all[source, c], down_buf[pl.ds(start, step), :], preferred_element_type=F32
        )
        total = term if total is None else total + term
    hid_copies = list(hid_copies.values())
    sent += hid_copies
    for i in range(ep_count):
        back[i] = total[i * slots : (i + 1) * slots, :].astype(BF16)
    back_copies = []
    for k in range(1, ep_count):
        to = lax.rem(ep_at + k, ep_count)
        back_copies.append(
            send(back.at[to], returned.at[ep_at], back_send, back_recv, k, (to, tp_at))
        )
    returned[ep_at] = back[ep_at]
    for copy in back_copies:
        copy.wait_recv()
    sent += back_copies
    results = merged(returned, ep_count)
    routed = jnp.dot(
        mixing, results, precision=lax.Precision.HIGHEST, preferred_element_type=F32
    )
    own = residual_buf[:, pl.ds(pl.multiple_of(tp_at * own_width, own_width), own_width)]
    out_tokens[...] = (own + routed).astype(BF16)
    for copy in sent:
        copy.wait_send()


def hand_on(count, *refs):
    sems = refs[2 * count]
    copies = [
        pltpu.make_async_copy(refs[i], refs[count + i], sems.at[i]) for i in range(count)
    ]
    for copy in copies:
        copy.start()
    for copy in copies:
        copy.wait()


def shards(
    tokens,
    mix_gain,
    w_query,
    w_key,
    w_value,
    w_igate,
    w_fgate,
    forget_bias,
    w_out,
    mem_state,
    norm_state,
    max_state,
    ffn_gain,
    route_ids,
    route_weights,
    w_gate,
    w_up,
    w_down,
):
    seqs, width = tokens.shape
    heads = mem_state.shape[1]
    head_dim = norm_state.shape[1] // heads
    tp_count = lax.axis_size("tp")
    ep_count = lax.axis_size("ep")
    own_width = width // tp_count
    top_count = route_ids.shape[1]
    span = FF // w_down.shape[0]
    experts = ep_count // span
    slot_cap = max(2, 3 * seqs * top_count // (2 * experts))
    slots = slot_cap
    memory = mem_state.reshape(seqs, heads, head_dim, head_dim)
    total = ep_count * slots
    units = w_gate.shape[1]
    step = min(256, units)
    vmem = pl.BlockSpec(memory_space=pltpu.VMEM)
    smem = pl.BlockSpec(memory_space=pltpu.SMEM)
    dma = pltpu.SemaphoreType.DMA
    outs = pl.pallas_call(
        functools.partial(kernel, (tp_count, ep_count, span, experts, slots, heads)),
        out_shape=(
            pltpu.VMEM((seqs, own_width), BF16),
            pltpu.VMEM(memory.shape, F32),
            pltpu.VMEM(norm_state.shape, F32),
            pltpu.VMEM((heads, seqs), F32),
        ),
        in_specs=[vmem] * 4 + [smem] + [vmem] * 5 + [pl.BlockSpec(memory_space=pltpu.HBM)] * 8,
        out_specs=(vmem,) * 4,
        scratch_shapes=[
            pltpu.VMEM((3,) + w_query.shape, BF16),
            pltpu.VMEM(w_out.shape, BF16),
            pltpu.VMEM(w_gate.shape, BF16),
            pltpu.VMEM(w_up.shape, BF16),
            pltpu.VMEM(w_down.shape, BF16),
            pltpu.VMEM((tp_count, seqs, width), BF16),
            pltpu.VMEM((seqs, width), F32),
            pltpu.VMEM((experts, slots, width), BF16),
            pltpu.VMEM((ep_count, slots, width), BF16),
            pltpu.VMEM((tp_count, units // step, total, step), BF16),
            pltpu.VMEM((ep_count, slots, own_width), BF16),
            pltpu.VMEM((ep_count, slots, own_width), BF16),
            dma((8,)),
            dma((tp_count,)),
            dma((tp_count,)),
            dma((ep_count,)),
            dma((ep_count,)),
            dma((tp_count * (units // step),)),
            dma((tp_count * (units // step),)),
            dma((ep_count,)),
            dma((ep_count,)),
        ],
        compiler_params=pltpu.CompilerParams(
            collective_id=0, has_side_effects=True, vmem_limit_bytes=67043328 - 600 * 1024
        ),
    )(
        tokens,
        mix_gain,
        w_igate.T,
        w_fgate.T,
        forget_bias,
        norm_state,
        max_state.T,
        ffn_gain,
        route_ids.T,
        route_weights.T,
        w_query,
        w_key,
        w_value,
        w_out,
        memory,
        w_gate,
        w_up,
        w_down,
    )
    outs = pl.pallas_call(
        functools.partial(hand_on, len(outs)),
        out_shape=tuple(jax.ShapeDtypeStruct(o.shape, o.dtype) for o in outs),
        in_specs=[vmem] * len(outs),
        out_specs=(pl.BlockSpec(memory_space=pltpu.HBM),) * len(outs),
        scratch_shapes=[dma((len(outs),))],
        compiler_params=pltpu.CompilerParams(vmem_limit_bytes=4 * 1024 * 1024),
    )(*outs)
    return outs[0], outs[1].reshape(mem_state.shape), outs[2], outs[3].T


def solution(mesh):
    placed = (
        P("ep", None),
        P(),
        P(None, "tp"),
        P(None, "tp"),
        P(None, "tp"),
        P(),
        P(),
        P(),
        P("tp", None),
        P("ep", "tp", None),
        P("ep", "tp"),
        P("ep", "tp"),
        P(),
        P("ep", None),
        P("ep", None),
        P(None, ("ep", "tp")),
        P(None, ("ep", "tp")),
        P("ep", "tp"),
    )
    return jax.shard_map(
        shards,
        mesh=mesh,
        in_specs=placed,
        out_specs=(P("ep", "tp"), P("ep", "tp", None), P("ep", "tp"), P("ep", "tp")),
        check_vma=False,
    )
```
